32 devices in a mesh: grp: 2 (over y), fs: 4 (over z), tp: 4 (over x, core).
Axes of the slice: x: 2, y: 2, z: 4, core: 2. Of those that a mesh axis runs over, the one named last changes fastest.
Arguments:
- tokens: bfloat16 [6144, 2048], P(('grp', 'fs'), 'tp'), parts along dimension 0, may hold values from -6 to 6
- mix_gain: float32 [2048], replicated, may hold values from 0.1 to 1.9
- w_u: float32 [2048, 1024], P('fs', 'tp'), may hold values from -0.125 to 0.125
- w_v: float32 [2048, 1024], P('fs', 'tp'), may hold values from -0.125 to 0.125
- u_scale: float32 [1024], P('tp'), may hold values from 0.5 to 2
- v_scale: float32 [1024], P('tp'), may hold values from 0.5 to 2
- spatial: bfloat16 [8, 128, 128], P('tp'), may hold values from -0.5 to 0.5
- spatial_bias: float32 [8, 128], P('tp'), may hold values from 0.1 to 1.9
- w_mix: float32 [1024, 2048], P('tp', 'fs'), may hold values from -0.1875 to 0.1875
- mix_scale: float32 [1, 2048], P(None, 'fs'), may hold values from 0.5 to 2
- ffn_gain: float32 [2048], replicated, may hold values from 0.1 to 1.9
- w_gate: float32 [2048, 5632], P('fs', 'tp'), may hold values from -0.125 to 0.125
- w_up: float32 [2048, 5632], P('fs', 'tp'), may hold values from -0.125 to 0.125
- gate_scale: float32 [5632], P('tp'), may hold values from 0.5 to 2
- up_scale: float32 [5632], P('tp'), may hold values from 0.5 to 2
- w_down: float32 [5632, 2048], P('tp', 'fs'), may hold values from -0.078125 to 0.078125
- down_scale: float32 [1, 2048], P(None, 'fs'), may hold values from 0.5 to 2
Outputs:
- layer_out: bfloat16 [6144, 2048], P(('grp', 'fs'), 'tp'), parts along dimension 0
The draws below stay inside these ranges and needn't reach their ends.
There are 2 independent parts, one for each index of `grp`. The reference program is written for one: setup_inputs(seed, part) draws one part's arguments, and reference() takes and returns one part's arrays. A program takes and returns all parts, laid end to end along the dimension named above; an argument that names none is the same for every part. Nothing has to cross between parts.
All inputs are finite; a program needn't handle non-finite values.
Results may differ from the reference program's by a relative error of at most 0.024.
Values may be sent and summed in bfloat16 or wider, within the bound.
A program may use at most 128 MiB of HBM per device.

```python
import math
import jax
import jax.numpy as jnp
from jax import lax

D = 2048
SGD = 128
SG = 8
SW = 1024
FF = 5632
BLK = 128
TOKENS = 3072
N_TP = 4


def shard_levels(key, dims, shards, least, high):
    loudness = 1.0
    for position, shards_of in shards:
        steps = jax.random.uniform(jax.random.fold_in(jax.random.fold_in(key, 6), position), (shards_of,), jnp.float32, least / len(shards), high / len(shards))
        loudness = loudness * jnp.repeat(jnp.exp(steps), dims[position] // shards_of).reshape((-1,) + (1,) * (len(dims) - 1 - position))
    return loudness


def centred(rng, shape, scale, limit, cuts=(), dtype=jnp.bfloat16):
    drawn = scale * jax.random.normal(rng, shape, jnp.float32)
    if cuts:
        drawn = drawn * shard_levels(rng, shape, cuts, -0.22, 0.18)
    return jnp.clip(drawn, -limit, limit).astype(dtype)


def setup_inputs(seed: int = 0, part: int = 0) -> dict:
    splits = jax.random.split(jax.random.key(seed), 18)
    part_keys = jax.random.split(jax.random.fold_in(splits[17], part), 18)
    return {
        "tokens": centred(part_keys[0], (TOKENS, D), 1.0, 6.0, ((0, 4), (1, 4))),
        "mix_gain": jnp.clip(1.0 + 0.18 * jax.random.normal(splits[1], (D,), jnp.float32), 0.1, 1.9),
        "w_u": centred(splits[2], (D, SW), D ** -0.5, 0.125, ((0, 4), (1, 4)), jnp.float32),
        "w_v": centred(splits[3], (D, SW), D ** -0.5, 0.125, ((0, 4), (1, 4)), jnp.float32),
        "u_scale": jnp.clip(jnp.exp(math.log(2.0) - 1.3862944 * jax.random.uniform(splits[4], (SW,), jnp.float32) ** shard_levels(splits[4], (SW,), ((0, 4),), -0.2, 0.2)), 0.5, 2.0),
        "v_scale": jnp.clip(jnp.exp(math.log(2.0) - 1.3862944 * jax.random.uniform(splits[5], (SW,), jnp.float32) ** shard_levels(splits[5], (SW,), ((0, 4),), -0.2, 0.2)), 0.5, 2.0),
        "spatial": centred(splits[6], (SG, BLK, BLK), BLK ** -0.5, 0.5, ((0, 4),)),
        "spatial_bias": jnp.clip(1.0 + 0.18 * jax.random.normal(splits[7], (SG, BLK), jnp.float32), 0.1, 1.9),
        "w_mix": centred(splits[8], (SW, D), SW ** -0.5, 0.1875, ((0, 4), (1, 4)), jnp.float32),
        "mix_scale": jnp.clip(jnp.exp(math.log(2.0) - 1.3862944 * jax.random.uniform(splits[9], (1, D), jnp.float32) ** shard_levels(splits[9], (1, D), ((1, 4),), -0.2, 0.2)), 0.5, 2.0),
        "ffn_gain": jnp.clip(1.0 + 0.18 * jax.random.normal(splits[10], (D,), jnp.float32), 0.1, 1.9),
        "w_gate": centred(splits[11], (D, FF), D ** -0.5, 0.125, ((0, 4), (1, 4)), jnp.float32),
        "w_up": centred(splits[12], (D, FF), D ** -0.5, 0.125, ((0, 4), (1, 4)), jnp.float32),
        "gate_scale": jnp.clip(jnp.exp(math.log(2.0) - 1.3862944 * jax.random.uniform(splits[13], (FF,), jnp.float32) ** shard_levels(splits[13], (FF,), ((0, 4),), -0.2, 0.2)), 0.5, 2.0),
        "up_scale": jnp.clip(jnp.exp(math.log(2.0) - 1.3862944 * jax.random.uniform(splits[14], (FF,), jnp.float32) ** shard_levels(splits[14], (FF,), ((0, 4),), -0.2, 0.2)), 0.5, 2.0),
        "w_down": centred(splits[15], (FF, D), FF ** -0.5, 0.078125, ((0, 4), (1, 4)), jnp.float32),
        "down_scale": jnp.clip(jnp.exp(math.log(2.0) - 1.3862944 * jax.random.uniform(splits[16], (1, D), jnp.float32) ** shard_levels(splits[16], (1, D), ((1, 4),), -0.2, 0.2)), 0.5, 2.0),
    }


eps = 1e-06

def norm_rows(rows, gain):
    wide = rows.astype(jnp.float32)
    factor = lax.rsqrt(lax.optimization_barrier(jnp.mean(wide * wide, axis=1, keepdims=True)) + eps)
    return (wide * factor * gain).astype(jnp.bfloat16)

def sliced_sum(hidden, weight, scale):
    width = hidden.shape[1] // N_TP
    total = jnp.zeros((hidden.shape[0], weight.shape[1]), jnp.float32)
    weight_half = weight.astype(jnp.bfloat16)
    for index in range(N_TP):
        left = hidden[:, index * width:(index + 1) * width]
        right = weight_half[index * width:(index + 1) * width]
        term = jnp.dot(left, right, preferred_element_type=jnp.float32) * scale
        rounded = lax.optimization_barrier(term.astype(jnp.bfloat16))
        total = total + rounded.astype(jnp.float32)
    return total

def reference(tokens, mix_gain, w_u, w_v, u_scale, v_scale, spatial, spatial_bias, w_mix, mix_scale, ffn_gain, w_gate, w_up, gate_scale, up_scale, w_down, down_scale):
    normed_in = norm_rows(tokens, mix_gain)
    u_act = jax.nn.gelu(jnp.dot(normed_in, w_u.astype(jnp.bfloat16), preferred_element_type=jnp.float32) * u_scale, approximate=False)
    v_act = jax.nn.gelu(jnp.dot(normed_in, w_v.astype(jnp.bfloat16), preferred_element_type=jnp.float32) * v_scale, approximate=False).astype(jnp.bfloat16)
    count = tokens.shape[0]
    blocks = v_act.reshape(count // BLK, BLK, SG, SGD).astype(jnp.float32)
    causal = jnp.arange(BLK)[:, None] >= jnp.arange(BLK)[None, :]
    masked = jnp.where(causal[None], spatial.astype(jnp.float32), jnp.float32(0.0))
    spatial_out = jnp.einsum('gts,nsgc->ntgc', masked, blocks) + spatial_bias.T[None, :, :, None]
    gated = (u_act * spatial_out.reshape(count, SW)).astype(jnp.bfloat16)
    mixed = sliced_sum(gated, w_mix, mix_scale)
    resid = (tokens.astype(jnp.float32) + mixed).astype(jnp.bfloat16)
    normed_ffn = norm_rows(resid, ffn_gain)
    gate_val = jnp.dot(normed_ffn, w_gate.astype(jnp.bfloat16), preferred_element_type=jnp.float32) * gate_scale
    up_val = jnp.dot(normed_ffn, w_up.astype(jnp.bfloat16), preferred_element_type=jnp.float32) * up_scale
    act = (jax.nn.silu(gate_val) * up_val).astype(jnp.bfloat16)
    down_sum = sliced_sum(act, w_down, down_scale)
    return (resid.astype(jnp.float32) + down_sum).astype(jnp.bfloat16)
```

```python
import jax
import jax.numpy as jnp
from jax import lax
from jax.sharding import PartitionSpec as P

eps = 1e-06


def norm_rows(shard, gain):
    whole = lax.all_gather(shard, "tp", axis=1, tiled=True)
    wide = whole.astype(jnp.float32)
    factor = lax.rsqrt(jnp.mean(wide * wide, axis=1, keepdims=True) + eps)
    return (wide * factor * gain).astype(jnp.bfloat16)


def swap_gather(weight, axis):
    groups = lax.axis_size("grp")
    half = weight.shape[0] // groups
    mine = lax.axis_index("grp")
    piece = lax.dynamic_slice_in_dim(weight, mine * half, half, 0).astype(jnp.bfloat16)
    held = lax.all_gather(piece, "fs", axis=0)
    other = lax.ppermute(held, "grp", [(i, (i + 1) % groups) for i in range(groups)])
    first = jnp.where(mine == 0, held, other)
    second = jnp.where(mine == 0, other, held)
    whole = jnp.concatenate([first, second], axis=1)
    if axis == 0:
        return whole.reshape(-1, weight.shape[1])
    return whole.transpose(1, 0, 2).reshape(weight.shape[0], -1)


def project_pair(rows, first, second):
    return (
        jnp.dot(rows, swap_gather(first, 0), preferred_element_type=jnp.float32),
        jnp.dot(rows, swap_gather(second, 0), preferred_element_type=jnp.float32),
    )


def reduce_out(hidden, weight, scale):
    term = jnp.dot(hidden, weight, preferred_element_type=jnp.float32) * scale
    return lax.psum_scatter(
        term.astype(jnp.bfloat16), "tp", scatter_dimension=1, tiled=True
    ).astype(jnp.float32)


def local(
    tokens,
    mix_gain,
    w_u,
    w_v,
    u_scale,
    v_scale,
    spatial,
    spatial_bias,
    w_mix,
    mix_scale,
    ffn_gain,
    w_gate,
    w_up,
    gate_scale,
    up_scale,
    w_down,
    down_scale,
):
    scales = lax.all_gather(jnp.concatenate([mix_scale, down_scale], axis=0), "fs", axis=1, tiled=True)
    held = (swap_gather(w_mix, 1), scales[:1])
    normed_in = norm_rows(tokens, mix_gain)
    u_pre, v_pre = project_pair(normed_in, w_u, w_v)
    u_act = jax.nn.gelu(u_pre * u_scale, approximate=False)
    v_act = jax.nn.gelu(v_pre * v_scale, approximate=False).astype(jnp.bfloat16)
    groups = spatial.shape[0]
    span = spatial.shape[1]
    count = v_act.shape[0]
    blocks = v_act.reshape(count // span, span, groups, v_act.shape[1] // groups)
    later = lax.broadcasted_iota(jnp.int32, (span, span), 0)
    earlier = lax.broadcasted_iota(jnp.int32, (span, span), 1)
    masked = jnp.where((later >= earlier)[None], spatial, jnp.zeros((), jnp.bfloat16))
    spatial_out = jnp.einsum("gts,nsgc->ntgc", masked, blocks, preferred_element_type=jnp.float32)
    spatial_out = spatial_out + spatial_bias.T[None, :, :, None]
    gated = (u_act * spatial_out.reshape(count, v_act.shape[1])).astype(jnp.bfloat16)
    mixed = reduce_out(gated, held[0], held[1])
    resid = (tokens.astype(jnp.float32) + mixed).astype(jnp.bfloat16)
    down_weight, down_factor = swap_gather(w_down, 1), scales[1:]
    normed_ffn = norm_rows(resid, ffn_gain)
    gate_pre, up_pre = project_pair(normed_ffn, w_gate, w_up)
    act = (jax.nn.silu(gate_pre * gate_scale) * (up_pre * up_scale)).astype(jnp.bfloat16)
    down_sum = reduce_out(act, down_weight, down_factor)
    return (resid.astype(jnp.float32) + down_sum).astype(jnp.bfloat16)


def solution(mesh):
    placed = (
        P(("grp", "fs"), "tp"),
        P(),
        P("fs", "tp"),
        P("fs", "tp"),
        P("tp"),
        P("tp"),
        P("tp", None, None),
        P("tp", None),
        P("tp", "fs"),
        P(None, "fs"),
        P(),
        P("fs", "tp"),
        P("fs", "tp"),
        P("tp"),
        P("tp"),
        P("tp", "fs"),
        P(None, "fs"),
    )
    return jax.shard_map(
        local, mesh=mesh, in_specs=placed, out_specs=P(("grp", "fs"), "tp"), check_vma=False
    )
```

```python
import functools

import jax
import jax.numpy as jnp
from jax import lax
from jax.experimental import pallas as pl
from jax.experimental.pallas import tpu as pltpu
from jax.sharding import PartitionSpec as P

MESH = pl.DeviceIdType.MESH
eps = 1e-06
H = 2
half_root = 0.7071067811865476


def gelu(a):
    return 0.5 * a * (1.0 + lax.erf(a * half_root))


def layer_kernel(
    dims,
    tokens,
    mix_gain,
    w_uv,
    w_mix,
    w_gate,
    w_up,
    w_down,
    u_scale,
    v_scale,
    spatial,
    bias,
    scales,
    ffn_gain,
    gate_scale,
    up_scale,
    out,
    uv_buf,
    mix_buf,
    gate_buf,
    up_buf,
    down_buf,
    scale_buf,
    tok_buf,
    res_buf,
    normed,
    gated,
    silu_buf,
    act,
    resid,
    give_buf,
    send_buf,
    pair_buf,
    far_buf,
    keep,
    z_send,
    z_recv,
    y_send,
    y_recv,
    w_local,
    s_send,
    s_recv,
    s_local,
    g_send,
    g_fwd,
    g_recv,
    g_local,
    p_send,
    p_recv,
    f_send,
    f_recv,
):
    n, n_tp = dims
    nx = n_tp // 2
    i = lax.axis_index("fs")
    g = lax.axis_index("grp")
    t = lax.axis_index("tp")
    x, c = t // 2, t % 2
    rows, dt = tokens.shape
    df = scales.shape[1]
    per = dt // df
    rt = rows // H
    partner = {"tp": x * 2 + 1 - c}
    across = {"grp": 1 - g}

    def remote(src, dst, ss, rs, device):
        return pltpu.make_async_remote_copy(
            src_ref=src,
            dst_ref=dst,
            send_sem=ss,
            recv_sem=rs,
            device_id=device,
            device_id_type=MESH,
        )

    barrier = pltpu.get_barrier_semaphore()
    for k in range(1, n):
        pl.semaphore_signal(barrier, 1, device_id={"fs": (i + k) % n}, device_id_type=MESH)
    pl.semaphore_signal(barrier, 1, device_id=across, device_id_type=MESH)
    pl.semaphore_signal(barrier, 1, device_id=partner, device_id_type=MESH)
    for k in range(1, nx):
        pl.semaphore_signal(
            barrier, 1, device_id={"tp": ((x + k) % nx) * 2 + c}, device_id_type=MESH
        )
    pl.semaphore_wait(barrier, (n - 1) + 2 + (nx - 1))

    cut = w_down.shape[0] // 2
    streams = (
        (w_uv, uv_buf, 0, w_uv.shape[0]),
        (w_mix, mix_buf, 0, w_mix.shape[0]),
        (w_gate, gate_buf, 0, w_gate.shape[0]),
        (w_up, up_buf, 0, w_up.shape[0]),
        (w_down, down_buf, 0, cut),
        (w_down, down_buf, cut, cut),
    )
    UV, MIX, GATE, UP, DOWN_A, DOWN_B = range(6)

    def part(k, who):
        half = streams[k][3] // 2
        return pl.ds(pl.multiple_of(streams[k][2] + who * half, 16), half)

    def z_copy(k, j, step, own):
        src, buf = streams[k][:2]
        sl = part(k, g)
        dst = buf.at[j, sl, :]
        slot = n if (own and step < 0) else j
        return remote(
            src.at[sl, :] if own else dst,
            dst,
            z_send.at[k, slot],
            z_recv.at[k, j],
            {"fs": jnp.clip(i + step, 0, n - 1)},
        )

    def y_copy(k, j, who):
        dst = streams[k][1].at[j, part(k, who), :]
        return remote(dst, dst, y_send.at[k, j], y_recv.at[k, j], across)

    def local_copy(k):
        src, buf, r0, count = streams[k]
        sl = pl.ds(r0, count)
        return pltpu.make_async_copy(src.at[sl, :], buf.at[i, sl, :], w_local.at[k])

    def own(k):
        @pl.when(i + 1 < n)
        def _():
            z_copy(k, i, 1, True).start()

        @pl.when(i > 0)
        def _():
            z_copy(k, i, -1, True).start()

    def service(k, s):
        left, right = i - s, i + s

        @pl.when(left >= 0)
        def _():
            z_copy(k, left, 1, False).wait_recv()

            @pl.when(i + 1 < n)
            def _():
                z_copy(k, left, 1, False).start()

            y_copy(k, left, g).start()

        @pl.when(right < n)
        def _():
            z_copy(k, right, -1, False).wait_recv()

            @pl.when(i > 0)
            def _():
                z_copy(k, right, -1, False).start()

            y_copy(k, right, g).start()

    def finish(k):
        local_copy(k).wait()
        for s in range(1, n):
            y_copy(k, lax.rem(i + s, n), 1 - g).wait_recv()

    def drain(k):
        @pl.when(i + 1 < n)
        def _():
            z_copy(k, i, 1, True).wait_send()

        @pl.when(i > 0)
        def _():
            z_copy(k, i, -1, True).wait_send()

        for s in range(1, n):
            j = lax.rem(i + s, n)
            y_copy(k, j, g).wait_send()

            @pl.when(jnp.logical_and(j < i, i + 1 < n))
            def _():
                z_copy(k, j, 1, False).wait_send()

            @pl.when(jnp.logical_and(j > i, i > 0))
            def _():
                z_copy(k, j, -1, False).wait_send()

    def scale_copy(s, mine):
        j = i if mine else lax.rem(i + s, n)
        return remote(
            scales,
            scale_buf.at[j],
            s_send.at[s],
            s_recv.at[j],
            {"fs": lax.rem(i + s, n)},
        )

    def chunk(h):
        return pl.ds(h * rt, rt)

    def far(k):
        return lax.rem(x + k, nx)

    def ag_x(r, src, buf, k, h):
        return remote(
            src.at[chunk(h), :],
            buf.at[t, chunk(h), :],
            g_send.at[r, k, h],
            g_recv.at[r, t, h],
            {"tp": far(k) * 2 + c} if k else partner,
        )

    def ag_in(r, buf, slot, h):
        ref = buf.at[slot, chunk(h), :]
        return remote(ref, ref, g_fwd.at[r, 0, h], g_recv.at[r, slot, h], partner)

    def ag_fwd(r, buf, k, h):
        slot = far(k) * 2 + c
        ref = buf.at[slot, chunk(h), :]
        return remote(ref, ref, g_fwd.at[r, k, h], g_recv.at[r, slot, h], partner)

    def ag_local(r, src, buf):
        return pltpu.make_async_copy(src, buf.at[t], g_local.at[r])

    def ag_start(r, src, buf):
        for h in range(H):
            for k in list(range(1, nx)) + [0]:
                ag_x(r, src, buf, k, h).start()
        ag_local(r, src, buf).start()

    def ag_finish(r, src, buf):
        for h in range(H):
            for k in range(1, nx):
                ag_fwd(r, buf, k, h).wait_recv()
                ag_fwd(r, buf, k, h).start()
        for h in range(H):
            for k in range(nx):
                ag_in(r, buf, far(k) * 2 + 1 - c, h).wait_recv()
        ag_local(r, src, buf).wait()

    def ag_drain(r, src, buf):
        for h in range(H):
            for k in range(nx):
                ag_x(r, src, buf, k, h).wait_send()
            for k in range(1, nx):
                ag_fwd(r, buf, k, h).wait_send()

    def norm(buf, gain):
        tile = 128

        def body(b, carry):
            sl = pl.ds(pl.multiple_of(b * tile, tile), tile)
            total = jnp.zeros((tile, 1), jnp.float32)
            for q in range(n_tp):
                wide = buf[q, sl, :].astype(jnp.float32)
                total = total + jnp.sum(wide * wide, axis=1, keepdims=True)
            factor = lax.rsqrt(total / (n_tp * dt) + eps)
            for q in range(n_tp):
                cols = slice(q * dt, (q + 1) * dt)
                wide = buf[q, sl, :].astype(jnp.float32)
                normed[sl, cols] = (wide * factor * gain[:, cols]).astype(jnp.bfloat16)
            return carry

        lax.fori_loop(0, rows // tile, body, 0)

    def pair_copy(r, xo, h):
        return remote(
            give_buf.at[xo, chunk(h), :],
            pair_buf.at[r, xo, chunk(h), :],
            p_send.at[r, xo, h],
            p_recv.at[r, xo, h],
            partner,
        )

    def far_copy(r, xo, h, slot):
        return remote(
            send_buf.at[xo, chunk(h), :],
            far_buf.at[r, slot, chunk(h), :],
            f_send.at[r, xo, h],
            f_recv.at[r, slot, h],
            {"tp": xo * 2 + c},
        )

    def reduce_over_tp(r, hidden, buf, scale_row, hook):
        def partial(owner, h):
            ws = [buf[owner * per + q] for q in range(per)]
            ss = [scale_buf[owner * per + q, scale_row : scale_row + 1, :] for q in range(per)]
            w = ws[0] if per == 1 else jnp.concatenate(ws, axis=1)
            s = ss[0] if per == 1 else jnp.concatenate(ss, axis=1)
            return jnp.dot(hidden[chunk(h), :], w, preferred_element_type=jnp.float32) * s

        for k in range(1, nx + 1):
            xo = far(k)
            for h in range(H):
                give_buf[xo, chunk(h), :] = partial(xo * 2 + 1 - c, h).astype(jnp.bfloat16)
                keep[xo, chunk(h), :] = partial(xo * 2 + c, h)
                pair_copy(r, xo, h).start()
            for h in range(H):
                pair_copy(r, xo, h).wait_recv()
                both = keep[xo, chunk(h), :] + pair_buf[r, xo, chunk(h), :].astype(jnp.float32)
                if k < nx:
                    send_buf[xo, chunk(h), :] = both.astype(jnp.bfloat16)
                else:
                    keep[xo, chunk(h), :] = both
            if k < nx:
                for h in range(H):
                    far_copy(r, xo, h, x).start()
        hook()

    def reduced(r, h):
        total = keep[x, chunk(h), :]
        for k in range(1, nx):
            far_copy(r, far(k), h, far(k)).wait_recv()
            total = total + far_buf[r, far(k), chunk(h), :].astype(jnp.float32)
        return total

    def reduce_drain(r):
        for k in range(1, nx + 1):
            for h in range(H):
                pair_copy(r, far(k), h).wait_send()
                if k < nx:
                    far_copy(r, far(k), h, x).wait_send()

    own(UV)
    own(MIX)
    ag_start(0, tokens, tok_buf)
    for s in range(1, n):
        scale_copy(s, True).start()
    own_scale = pltpu.make_async_copy(scales, scale_buf.at[i], s_local)
    own_scale.start()
    for k in range(6):
        local_copy(k).start()
    for s in range(1, n):
        service(UV, s)
        service(MIX, s)
    own(GATE)
    own(UP)
    ag_finish(0, tokens, tok_buf)
    norm(tok_buf, mix_gain)
    own_scale.wait()
    for s in range(1, n):
        scale_copy(s, False).wait_recv()
    finish(UV)

    groups, span = spatial.shape[0], spatial.shape[1]
    width = u_scale.shape[1]
    wide = width // groups
    causal = lax.broadcasted_iota(jnp.int32, (span, span), 0) >= lax.broadcasted_iota(
        jnp.int32, (span, span), 1
    )
    uv_w = uv_buf[...].reshape(-1, 2 * width)
    for h in range(H):
        pre = jnp.dot(normed[chunk(h), :], uv_w, preferred_element_type=jnp.float32)
        u = gelu(pre[:, :width] * u_scale[...])
        v = gelu(pre[:, width:] * v_scale[...]).astype(jnp.bfloat16)
        for q in range(groups):
            m = jnp.where(causal, spatial[q].astype(jnp.float32), 0.0).astype(jnp.bfloat16)
            cols = slice(q * wide, (q + 1) * wide)
            for b in range(rt // span):
                sl = slice(b * span, (b + 1) * span)
                mixed = jnp.dot(m, v[sl, cols], preferred_element_type=jnp.float32)
                mixed = mixed + bias[:, q : q + 1]
                gated[h * rt + b * span : h * rt + (b + 1) * span, cols] = (
                    u[sl, cols] * mixed
                ).astype(jnp.bfloat16)
    finish(MIX)

    def after_mix():
        service(GATE, 1)
        own(DOWN_A)

    reduce_over_tp(0, gated, mix_buf, 0, after_mix)
    for h in range(H):
        resid[chunk(h), :] = (
            tokens[chunk(h), :].astype(jnp.float32) + reduced(0, h)
        ).astype(jnp.bfloat16)
    ag_start(1, resid, res_buf)
    reduce_drain(0)
    for s in range(2, n):
        service(GATE, s)
    ag_finish(1, resid, res_buf)
    norm(res_buf, ffn_gain)
    for s in range(1, n):
        service(UP, s)
    own(DOWN_B)
    finish(GATE)


    ff = gate_scale.shape[1]
    gt = rows // 4

    def gate_step(b, carry):
        sl = pl.ds(pl.multiple_of(b * gt, 64), gt)
        a = jnp.dot(
            normed[sl, :], gate_buf[...].reshape(-1, ff), preferred_element_type=jnp.float32
        )
        a = a * gate_scale[...]
        silu_buf[sl, :] = a / (1.0 + jnp.exp(-a))
        return carry

    lax.fori_loop(0, 4, gate_step, 0)
    for s in range(1, n):
        service(DOWN_A, s)
    finish(UP)

    def up_step(b, carry):
        sl = pl.ds(pl.multiple_of(b * gt, 64), gt)
        a = jnp.dot(
            normed[sl, :], up_buf[...].reshape(-1, ff), preferred_element_type=jnp.float32
        )
        act[sl, :] = (silu_buf[sl, :] * (a * up_scale[...])).astype(jnp.bfloat16)
        return carry

    lax.fori_loop(0, 4, up_step, 0)
    for s in range(1, n):
        service(DOWN_B, s)
    finish(DOWN_A)
    finish(DOWN_B)
    reduce_over_tp(1, act, down_buf, 8, lambda: None)
    for h in range(H):
        out[chunk(h), :] = (
            resid[chunk(h), :].astype(jnp.float32) + reduced(1, h)
        ).astype(jnp.bfloat16)
    reduce_drain(1)
    ag_drain(0, tokens, tok_buf)
    ag_drain(1, resid, res_buf)
    for k in range(6):
        drain(k)
    for s in range(1, n):
        scale_copy(s, True).wait_send()


def local(
    dims,
    tokens,
    mix_gain,
    w_u,
    w_v,
    u_scale,
    v_scale,
    spatial,
    spatial_bias,
    w_mix,
    mix_scale,
    ffn_gain,
    w_gate,
    w_up,
    gate_scale,
    up_scale,
    w_down,
    down_scale,
):
    n, n_tp = dims
    nx = n_tp // 2
    half = jnp.bfloat16
    rows, dt = tokens.shape
    df = mix_scale.shape[1]
    scales = jnp.concatenate(
        [jnp.broadcast_to(mix_scale, (8, df)), jnp.broadcast_to(down_scale, (8, df))], axis=0
    )
    w_uv = jnp.concatenate([w_u, w_v], axis=1).astype(half)
    hbm = pl.BlockSpec(memory_space=pl.ANY)
    vmem = pl.BlockSpec(memory_space=pltpu.VMEM)
    ff = w_gate.shape[1]
    dma = pltpu.SemaphoreType.DMA
    return pl.pallas_call(
        functools.partial(layer_kernel, dims),
        out_shape=jax.ShapeDtypeStruct((rows, dt), half),
        in_specs=[vmem, vmem] + [hbm] * 5 + [vmem] * 8,
        out_specs=vmem,
        scratch_shapes=[
            pltpu.VMEM((n,) + w_uv.shape, half),
            pltpu.VMEM((n,) + w_mix.shape, half),
            pltpu.VMEM((n,) + w_gate.shape, half),
            pltpu.VMEM((n,) + w_up.shape, half),
            pltpu.VMEM((n,) + w_down.shape, half),
            pltpu.VMEM((n,) + scales.shape, jnp.float32),
            pltpu.VMEM((n_tp, rows, dt), half),
            pltpu.VMEM((n_tp, rows, dt), half),
            pltpu.VMEM((rows, n_tp * dt), half),
            pltpu.VMEM((rows, w_u.shape[1]), half),
            pltpu.VMEM((rows, ff), jnp.float32),
            pltpu.VMEM((rows, ff), half),
            pltpu.VMEM((rows, dt), half),
            pltpu.VMEM((nx, rows, dt), half),
            pltpu.VMEM((nx, rows, dt), half),
            pltpu.VMEM((2, nx, rows, dt), half),
            pltpu.VMEM((2, nx, rows, dt), half),
            pltpu.VMEM((nx, rows, dt), jnp.float32),
            dma((6, n + 1)),
            dma((6, n)),
            dma((6, n)),
            dma((6, n)),
            dma((6,)),
            dma((n,)),
            dma((n,)),
            dma,
            dma((2, nx, H)),
            dma((2, nx, H)),
            dma((2, n_tp, H)),
            dma((2,)),
            dma((2, nx, H)),
            dma((2, nx, H)),
            dma((2, nx, H)),
            dma((2, nx, H)),
        ],
        compiler_params=pltpu.CompilerParams(
            collective_id=0, has_side_effects=True, vmem_limit_bytes=66000000
        ),
    )(
        tokens,
        mix_gain[None],
        w_uv,
        w_mix.astype(half),
        w_gate.astype(half),
        w_up.astype(half),
        w_down.astype(half),
        u_scale[None],
        v_scale[None],
        spatial,
        spatial_bias.T,
        scales,
        ffn_gain[None],
        gate_scale[None],
        up_scale[None],
    )


def solution(mesh):
    placed = (
        P(("grp", "fs"), "tp"),
        P(),
        P("fs", "tp"),
        P("fs", "tp"),
        P("tp"),
        P("tp"),
        P("tp", None, None),
        P("tp", None),
        P("tp", "fs"),
        P(None, "fs"),
        P(),
        P("fs", "tp"),
        P("fs", "tp"),
        P("tp"),
        P("tp"),
        P("tp", "fs"),
        P(None, "fs"),
    )
    dims = (mesh.shape["fs"], mesh.shape["tp"])
    return jax.shard_map(
        functools.partial(local, dims),
        mesh=mesh,
        in_specs=placed,
        out_specs=P(("grp", "fs"), "tp"),
        check_vma=False,
    )
```

```python
import functools

import jax
import jax.numpy as jnp
from jax import lax
from jax.experimental import pallas as pl
from jax.experimental.pallas import tpu as pltpu
from jax.sharding import PartitionSpec as P

MESH = pl.DeviceIdType.MESH
eps = 1e-06
H = 2
half_root = 0.7071067811865476


def gelu(a):
    return 0.5 * a * (1.0 + lax.erf(a * half_root))


def layer_kernel(
    dims,
    tokens,
    gains,
    w_uv,
    w_mix,
    w_gate,
    w_up,
    w_down,
    uv_scale,
    spatial,
    bias,
    scales,
    ffn_scale,
    out,
    uv_buf,
    mix_buf,
    gate_buf,
    up_buf,
    down_buf,
    scale_buf,
    tok_buf,
    res_buf,
    normed,
    gated,
    silu_buf,
    act,
    resid,
    give_buf,
    send_buf,
    pair_buf,
    far_buf,
    keep,
    z_send,
    z_recv,
    y_send,
    y_recv,
    w_local,
    s_send,
    s_recv,
    s_local,
    g_send,
    g_fwd,
    g_recv,
    g_local,
    p_send,
    p_recv,
    f_send,
    f_recv,
):
    n, n_tp = dims
    nx = n_tp // 2
    i = lax.axis_index("fs")
    g = lax.axis_index("grp")
    t = lax.axis_index("tp")
    x, c = t // 2, t % 2
    rows, dt = tokens.shape
    df = scales.shape[1]
    per = dt // df
    rt = rows // H
    partner = {"tp": x * 2 + 1 - c}
    across = {"grp": 1 - g}

    def remote(src, dst, ss, rs, device):
        return pltpu.make_async_remote_copy(
            src_ref=src,
            dst_ref=dst,
            send_sem=ss,
            recv_sem=rs,
            device_id=device,
            device_id_type=MESH,
        )

    barrier = pltpu.get_barrier_semaphore()
    for k in range(1, n):
        pl.semaphore_signal(barrier, 1, device_id={"fs": (i + k) % n}, device_id_type=MESH)
    pl.semaphore_signal(barrier, 1, device_id=across, device_id_type=MESH)
    pl.semaphore_signal(barrier, 1, device_id=partner, device_id_type=MESH)
    for k in range(1, nx):
        pl.semaphore_signal(
            barrier, 1, device_id={"tp": ((x + k) % nx) * 2 + c}, device_id_type=MESH
        )
    pl.semaphore_wait(barrier, (n - 1) + 2 + (nx - 1))

    units = w_down.shape[0] // 32
    first = units // 2
    second = (units - first + 1) // 2
    ends = (0, first * 32, (first + second) * 32, w_down.shape[0])
    streams = (
        (w_uv, uv_buf, 0, w_uv.shape[0]),
        (w_mix, mix_buf, 0, w_mix.shape[0]),
        (w_gate, gate_buf, 0, w_gate.shape[0]),
        (w_up, up_buf, 0, w_up.shape[0]),
    ) + tuple((w_down, down_buf, ends[q], ends[q + 1] - ends[q]) for q in range(3))
    UV, MIX, GATE, UP, DOWN_A, DOWN_B, DOWN_C = range(7)

    def part(k, who):
        half = streams[k][3] // 2
        return pl.ds(pl.multiple_of(streams[k][2] + who * half, 16), half)

    def z_copy(k, j, step, own):
        src, buf = streams[k][:2]
        sl = part(k, g)
        dst = buf.at[j, sl, :]
        slot = n if (own and step < 0) else j
        return remote(
            src.at[sl, :] if own else dst,
            dst,
            z_send.at[k, slot],
            z_recv.at[k, j],
            {"fs": jnp.clip(i + step, 0, n - 1)},
        )

    def y_copy(k, j, who):
        dst = streams[k][1].at[j, part(k, who), :]
        return remote(dst, dst, y_send.at[k, j], y_recv.at[k, j], across)

    def local_copy(k):
        src, buf, r0, count = streams[k]
        sl = pl.ds(r0, count)
        return pltpu.make_async_copy(src.at[sl, :], buf.at[i, sl, :], w_local.at[k])

    def own(k):
        @pl.when(i + 1 < n)
        def _():
            z_copy(k, i, 1, True).start()

        @pl.when(i > 0)
        def _():
            z_copy(k, i, -1, True).start()

    def service(k, s):
        left, right = i - s, i + s

        @pl.when(left >= 0)
        def _():
            z_copy(k, left, 1, False).wait_recv()

            @pl.when(i + 1 < n)
            def _():
                z_copy(k, left, 1, False).start()

            y_copy(k, left, g).start()

        @pl.when(right < n)
        def _():
            z_copy(k, right, -1, False).wait_recv()

            @pl.when(i > 0)
            def _():
                z_copy(k, right, -1, False).start()

            y_copy(k, right, g).start()

    def run(k, begin, end):
        for s in range(begin, min(end, n)):
            service(k, s)

    def finish(k):
        local_copy(k).wait()
        for s in range(1, n):
            y_copy(k, lax.rem(i + s, n), 1 - g).wait_recv()

    def drain(k):
        @pl.when(i + 1 < n)
        def _():
            z_copy(k, i, 1, True).wait_send()

        @pl.when(i > 0)
        def _():
            z_copy(k, i, -1, True).wait_send()

        for s in range(1, n):
            j = lax.rem(i + s, n)
            y_copy(k, j, g).wait_send()

            @pl.when(jnp.logical_and(j < i, i + 1 < n))
            def _():
                z_copy(k, j, 1, False).wait_send()

            @pl.when(jnp.logical_and(j > i, i > 0))
            def _():
                z_copy(k, j, -1, False).wait_send()

    def scale_copy(s, mine):
        j = i if mine else lax.rem(i + s, n)
        return remote(
            scales,
            scale_buf.at[j],
            s_send.at[s],
            s_recv.at[j],
            {"fs": lax.rem(i + s, n)},
        )

    def chunk(h):
        return pl.ds(h * rt, rt)

    def far(k):
        return lax.rem(x + k, nx)

    def ag_x(r, src, buf, k, h):
        return remote(
            src.at[chunk(h), :],
            buf.at[t, chunk(h), :],
            g_send.at[r, k, h],
            g_recv.at[r, t, h],
            {"tp": far(k) * 2 + c} if k else partner,
        )

    def ag_in(r, buf, slot, h):
        ref = buf.at[slot, chunk(h), :]
        return remote(ref, ref, g_fwd.at[r, 0, h], g_recv.at[r, slot, h], partner)

    def ag_fwd(r, buf, k, h):
        slot = far(k) * 2 + c
        ref = buf.at[slot, chunk(h), :]
        return remote(ref, ref, g_fwd.at[r, k, h], g_recv.at[r, slot, h], partner)

    def ag_local(r, src, buf):
        return pltpu.make_async_copy(src, buf.at[t], g_local.at[r])

    def ag_start(r, src, buf):
        for h in range(H):
            for k in list(range(1, nx)) + [0]:
                ag_x(r, src, buf, k, h).start()
        ag_local(r, src, buf).start()

    def ag_finish(r, src, buf):
        for h in range(H):
            for k in range(1, nx):
                ag_fwd(r, buf, k, h).wait_recv()
                ag_fwd(r, buf, k, h).start()
        for h in range(H):
            for k in range(nx):
                ag_in(r, buf, far(k) * 2 + 1 - c, h).wait_recv()
        ag_local(r, src, buf).wait()

    def ag_drain(r, src, buf):
        for h in range(H):
            for k in range(nx):
                ag_x(r, src, buf, k, h).wait_send()
            for k in range(1, nx):
                ag_fwd(r, buf, k, h).wait_send()

    def norm(buf, gain):
        tile = 128

        def body(b, carry):
            sl = pl.ds(pl.multiple_of(b * tile, tile), tile)
            total = jnp.zeros((tile, 1), jnp.float32)
            for q in range(n_tp):
                wide = buf[q, sl, :].astype(jnp.float32)
                total = total + jnp.sum(wide * wide, axis=1, keepdims=True)
            factor = lax.rsqrt(total / (n_tp * dt) + eps)
            for q in range(n_tp):
                cols = slice(q * dt, (q + 1) * dt)
                wide = buf[q, sl, :].astype(jnp.float32)
                normed[sl, cols] = (wide * factor * gain[:, cols]).astype(jnp.bfloat16)
            return carry

        lax.fori_loop(0, rows // tile, body, 0)

    def pair_copy(r, xo, h):
        return remote(
            give_buf.at[xo, chunk(h), :],
            pair_buf.at[r, xo, chunk(h), :],
            p_send.at[r, xo, h],
            p_recv.at[r, xo, h],
            partner,
        )

    def far_copy(r, xo, h, slot):
        return remote(
            send_buf.at[xo, chunk(h), :],
            far_buf.at[r, slot, chunk(h), :],
            f_send.at[r, xo, h],
            f_recv.at[r, slot, h],
            {"tp": xo * 2 + c},
        )

    def reduce_over_tp(r, hidden, buf, scale_row, hook):
        def partial(owner, h):
            ws = [buf[owner * per + q] for q in range(per)]
            ss = [scale_buf[owner * per + q, scale_row : scale_row + 1, :] for q in range(per)]
            w = ws[0] if per == 1 else jnp.concatenate(ws, axis=1)
            s = ss[0] if per == 1 else jnp.concatenate(ss, axis=1)
            return jnp.dot(hidden[chunk(h), :], w, preferred_element_type=jnp.float32) * s

        for k in range(1, nx + 1):
            xo = far(k)
            for h in range(H):
                give_buf[xo, chunk(h), :] = partial(xo * 2 + 1 - c, h).astype(jnp.bfloat16)
                keep[xo, chunk(h), :] = partial(xo * 2 + c, h)
                pair_copy(r, xo, h).start()
            for h in range(H):
                pair_copy(r, xo, h).wait_recv()
                both = keep[xo, chunk(h), :] + pair_buf[r, xo, chunk(h), :].astype(jnp.float32)
                if k < nx:
                    send_buf[xo, chunk(h), :] = both.astype(jnp.bfloat16)
                else:
                    keep[xo, chunk(h), :] = both
            if k < nx:
                for h in range(H):
                    far_copy(r, xo, h, x).start()
        hook()

    def reduced(r, h):
        total = keep[x, chunk(h), :]
        for k in range(1, nx):
            far_copy(r, far(k), h, far(k)).wait_recv()
            total = total + far_buf[r, far(k), chunk(h), :].astype(jnp.float32)
        return total

    def reduce_drain(r):
        for k in range(1, nx + 1):
            for h in range(H):
                pair_copy(r, far(k), h).wait_send()
                if k < nx:
                    far_copy(r, far(k), h, x).wait_send()

    own(UV)
    own(MIX)
    ag_start(0, tokens, tok_buf)
    for s in range(1, n):
        scale_copy(s, True).start()
    own_scale = pltpu.make_async_copy(scales, scale_buf.at[i], s_local)
    own_scale.start()
    for k in range(7):
        local_copy(k).start()
    for s in range(1, n):
        service(UV, s)
        service(MIX, s)
        if s == max(n - 2, 1):
            own(GATE)
            own(UP)
    ag_finish(0, tokens, tok_buf)
    norm(tok_buf, gains[0:1, :])
    own_scale.wait()
    for s in range(1, n):
        scale_copy(s, False).wait_recv()
    finish(UV)

    groups, span = spatial.shape[0], spatial.shape[1]
    width = uv_scale.shape[1]
    wide = width // groups
    causal = lax.broadcasted_iota(jnp.int32, (span, span), 0) >= lax.broadcasted_iota(
        jnp.int32, (span, span), 1
    )
    uv_w = uv_buf[...].reshape(-1, 2 * width)
    tilt = [jnp.broadcast_to(bias[q : q + 1, :], (span, span)).T[:, :1] for q in range(groups)]
    for h in range(H):
        pre = jnp.dot(normed[chunk(h), :], uv_w, preferred_element_type=jnp.float32)
        u = gelu(pre[:, :width] * uv_scale[0:1, :])
        v = gelu(pre[:, width:] * uv_scale[1:2, :]).astype(jnp.bfloat16)
        for q in range(groups):
            m = jnp.where(causal, spatial[q].astype(jnp.float32), 0.0).astype(jnp.bfloat16)
            cols = slice(q * wide, (q + 1) * wide)
            for b in range(rt // span):
                sl = slice(b * span, (b + 1) * span)
                mixed = jnp.dot(m, v[sl, cols], preferred_element_type=jnp.float32)
                mixed = mixed + tilt[q]
                gated[h * rt + b * span : h * rt + (b + 1) * span, cols] = (
                    u[sl, cols] * mixed
                ).astype(jnp.bfloat16)
    finish(MIX)

    def after_mix():
        service(GATE, 1)
        own(DOWN_A)

    reduce_over_tp(0, gated, mix_buf, 0, after_mix)
    for h in range(H):
        resid[chunk(h), :] = (
            tokens[chunk(h), :].astype(jnp.float32) + reduced(0, h)
        ).astype(jnp.bfloat16)
    ag_start(1, resid, res_buf)
    reduce_drain(0)
    run(UP, 1, 2)
    run(GATE, 2, 3)
    own(DOWN_B)
    ag_finish(1, resid, res_buf)
    norm(res_buf, gains[1:2, :])
    run(UP, 2, 3)
    run(GATE, 3, n)
    own(DOWN_C)
    run(DOWN_A, 1, 2)
    run(DOWN_B, 1, 2)
    finish(GATE)


    ff = ffn_scale.shape[1]
    gt = rows // 4

    def gate_step(b, carry):
        sl = pl.ds(pl.multiple_of(b * gt, 64), gt)
        a = jnp.dot(
            normed[sl, :], gate_buf[...].reshape(-1, ff), preferred_element_type=jnp.float32
        )
        a = a * ffn_scale[0:1, :]
        silu_buf[sl, :] = a / (1.0 + jnp.exp(-a))
        return carry

    lax.fori_loop(0, 4, gate_step, 0)
    run(UP, 3, n)
    run(DOWN_C, 1, 2)
    run(DOWN_A, 2, 3)
    run(DOWN_B, 2, 3)
    finish(UP)

    def up_step(b, carry):
        sl = pl.ds(pl.multiple_of(b * gt, 64), gt)
        a = jnp.dot(
            normed[sl, :], up_buf[...].reshape(-1, ff), preferred_element_type=jnp.float32
        )
        act[sl, :] = (silu_buf[sl, :] * (a * ffn_scale[1:2, :])).astype(jnp.bfloat16)
        return carry

    lax.fori_loop(0, 4, up_step, 0)
    run(DOWN_C, 2, 3)
    run(DOWN_A, 3, n)
    run(DOWN_B, 3, n)
    run(DOWN_C, 3, n)
    finish(DOWN_A)
    finish(DOWN_B)
    finish(DOWN_C)
    reduce_over_tp(1, act, down_buf, 8, lambda: None)
    for h in range(H):
        out[chunk(h), :] = (
            resid[chunk(h), :].astype(jnp.float32) + reduced(1, h)
        ).astype(jnp.bfloat16)
    reduce_drain(1)
    ag_drain(0, tokens, tok_buf)
    ag_drain(1, resid, res_buf)
    for k in range(7):
        drain(k)
    for s in range(1, n):
        scale_copy(s, True).wait_send()


def local(
    dims,
    tokens,
    mix_gain,
    w_u,
    w_v,
    u_scale,
    v_scale,
    spatial,
    spatial_bias,
    w_mix,
    mix_scale,
    ffn_gain,
    w_gate,
    w_up,
    gate_scale,
    up_scale,
    w_down,
    down_scale,
):
    n, n_tp = dims
    nx = n_tp // 2
    half = jnp.bfloat16
    rows, dt = tokens.shape
    df = mix_scale.shape[1]
    scales = jnp.concatenate(
        [jnp.broadcast_to(mix_scale, (8, df)), jnp.broadcast_to(down_scale, (8, df))], axis=0
    )
    w_uv = jnp.concatenate([w_u, w_v], axis=1).astype(half)
    hbm = pl.BlockSpec(memory_space=pl.ANY)
    vmem = pl.BlockSpec(memory_space=pltpu.VMEM)
    ff = w_gate.shape[1]
    dma = pltpu.SemaphoreType.DMA
    return pl.pallas_call(
        functools.partial(layer_kernel, dims),
        out_shape=jax.ShapeDtypeStruct((rows, dt), half),
        in_specs=[vmem, vmem] + [hbm] * 5 + [vmem] * 5,
        out_specs=vmem,
        scratch_shapes=[
            pltpu.VMEM((n,) + w_uv.shape, half),
            pltpu.VMEM((n,) + w_mix.shape, half),
            pltpu.VMEM((n,) + w_gate.shape, half),
            pltpu.VMEM((n,) + w_up.shape, half),
            pltpu.VMEM((n,) + w_down.shape, half),
            pltpu.VMEM((n,) + scales.shape, jnp.float32),
            pltpu.VMEM((n_tp, rows, dt), half),
            pltpu.VMEM((n_tp, rows, dt), half),
            pltpu.VMEM((rows, n_tp * dt), half),
            pltpu.VMEM((rows, w_u.shape[1]), half),
            pltpu.VMEM((rows, ff), jnp.float32),
            pltpu.VMEM((rows, ff), half),
            pltpu.VMEM((rows, dt), half),
            pltpu.VMEM((nx, rows, dt), half),
            pltpu.VMEM((nx, rows, dt), half),
            pltpu.VMEM((2, nx, rows, dt), half),
            pltpu.VMEM((2, nx, rows, dt), half),
            pltpu.VMEM((nx, rows, dt), jnp.float32),
            dma((7, n + 1)),
            dma((7, n)),
            dma((7, n)),
            dma((7, n)),
            dma((7,)),
            dma((n,)),
            dma((n,)),
            dma,
            dma((2, nx, H)),
            dma((2, nx, H)),
            dma((2, n_tp, H)),
            dma((2,)),
            dma((2, nx, H)),
            dma((2, nx, H)),
            dma((2, nx, H)),
            dma((2, nx, H)),
        ],
        compiler_params=pltpu.CompilerParams(
            collective_id=0, has_side_effects=True, vmem_limit_bytes=66000000
        ),
    )(
        tokens,
        jnp.stack([mix_gain, ffn_gain]),
        w_uv,
        w_mix.astype(half),
        w_gate.astype(half),
        w_up.astype(half),
        w_down.astype(half),
        jnp.stack([u_scale, v_scale]),
        spatial,
        spatial_bias,
        scales,
        jnp.stack([gate_scale, up_scale]),
    )


def solution(mesh):
    placed = (
        P(("grp", "fs"), "tp"),
        P(),
        P("fs", "tp"),
        P("fs", "tp"),
        P("tp"),
        P("tp"),
        P("tp", None, None),
        P("tp", None),
        P("tp", "fs"),
        P(None, "fs"),
        P(),
        P("fs", "tp"),
        P("fs", "tp"),
        P("tp"),
        P("tp"),
        P("tp", "fs"),
        P(None, "fs"),
    )
    dims = (mesh.shape["fs"], mesh.shape["tp"])
    return jax.shard_map(
        functools.partial(local, dims),
        mesh=mesh,
        in_specs=placed,
        out_specs=P(("grp", "fs"), "tp"),
        check_vma=False,
    )
```
